32 devices in a mesh: grp: 2 (over y), ep: 4 (over z), tp: 4 (over x, core).
Axes of the slice: x: 2, y: 2, z: 4, core: 2. Of those that a mesh axis runs over, the one named last changes fastest.
Arguments:
- mix_rows: bfloat16 [4096, 2048], P(('grp', 'ep', 'tp')), parts along dimension 0, may hold values from -6 to 6
- expert_rows: bfloat16 [4096, 2048], P(('grp', 'ep', 'tp')), parts along dimension 0, may hold values from -6 to 6
- mix_gain: float32 [2048], replicated, may hold values from 0.1 to 1.9
- ffn_gain: float32 [2048], replicated, may hold values from 0.1 to 1.9
- w_query: bfloat16 [2048, 512], P(None, 'tp'), may hold values from -0.125 to 0.125
- w_key: bfloat16 [2048, 512], P(None, 'tp'), may hold values from -0.125 to 0.125
- w_value: bfloat16 [2048, 1024], P(None, 'tp'), may hold values from -0.125 to 0.125
- w_lowrank: bfloat16 [2048, 32], replicated, may hold values from -0.125 to 0.125
- w_decay: bfloat16 [32, 512], replicated, may hold values from -1 to 1
- decay_bias: float32 [512], replicated, may hold values from -1.5 to 16
- decay_shift: float32 [8, 4096], P('tp', ('grp', 'ep')), parts along dimension 1, may hold values from -2 to 0
- head_gain: float32 [128], replicated, may hold values from 0.1 to 1.9
- w_output: bfloat16 [1024, 2048], P('tp'), may hold values from -0.1875 to 0.1875
- route_ids: int32 [4096, 4], P(('grp', 'ep', 'tp')), parts along dimension 0, may hold values from 0 to 15, all different within a row; in each aligned block of 128 rows (0 to 127, 128 to 255, ...) at most 64 rows name the same one
- route_weights: float32 [4096, 4], P(('grp', 'ep', 'tp')), parts along dimension 0, may hold values from 0.3 to 1.2
- w_gate: bfloat16 [16, 2048, 512], P(('ep', 'tp')), may hold values from -0.125 to 0.125
- w_lift: bfloat16 [16, 2048, 512], P(('ep', 'tp')), may hold values from -0.125 to 0.125
- w_drop: bfloat16 [16, 512, 2048], P(('ep', 'tp')), may hold values from -0.25 to 0.25
- shared_gate: bfloat16 [2048, 512], P(None, 'tp'), may hold values from -0.125 to 0.125
- shared_lift: bfloat16 [2048, 512], P(None, 'tp'), may hold values from -0.125 to 0.125
- shared_drop: bfloat16 [512, 2048], P('tp'), may hold values from -0.25 to 0.25
Outputs:
- mixed: bfloat16 [4096, 2048], P(('grp', 'ep', 'tp')), parts along dimension 0
- expert_out: bfloat16 [4096, 2048], P(('grp', 'ep', 'tp')), parts along dimension 0
The draws below stay inside these ranges and needn't reach their ends.
There are 2 independent parts, one for each index of `grp`. The reference program is written for one: setup_inputs(seed, part) draws one part's arguments, and reference() takes and returns one part's arrays. A program takes and returns all parts, laid end to end along the dimension named above; an argument that names none is the same for every part. Nothing has to cross between parts.
Inputs may be any that keep to these rules, and one draw needn't show every extreme that they name: `route_ids`: each row names 4 different experts. In each aligned block of 128 rows (the rows of one device) no expert is named by more than 64 rows.
All inputs are finite; a program needn't handle non-finite values.
Results may differ from the reference program's by a relative error of at most 0.014.
Values may be sent and summed in bfloat16 or wider, within the bound.
A program may use at most 128 MiB of HBM per device.

```python
import math
import jax
import jax.numpy as jnp
import numpy as np
from jax import lax

D = 2048
HEAD_COUNT = 8
DK = 64
DV = 128
LOWRANK = 32
BLOCK = 64
FF = 512
TOP_K = 4
TOK_DEV = 128
SPAN = 512
SEQUENCE_LENGTH = 2048
EXPERTS = 16
CAP = 64
N_EP = 4
N_TP = 4


def draw_decay_bias(key, part):
    key_sequence = jax.random.split(jax.random.fold_in(key, 7), 3)
    slow_share = 4
    slow_heads = jax.random.randint(key_sequence[0], (HEAD_COUNT,), 0, 8) < slow_share
    fast_bias = jax.random.uniform(key_sequence[1], (HEAD_COUNT, DK), jnp.float32, -1.5, 1.0)
    slow_floor = math.log(SEQUENCE_LENGTH) + 1.0
    slow_bias = slow_floor + jax.random.uniform(key_sequence[2], (HEAD_COUNT, DK), jnp.float32, 0.0, 1.0) * (16.0 - slow_floor)
    return jnp.where(slow_heads[:, None], slow_bias, fast_bias).reshape(HEAD_COUNT * DK).astype(jnp.float32)


def draw_decay_shift(key, part):
    key_sequence = jax.random.split(jax.random.fold_in(key, 13), 3)
    spans = SEQUENCE_LENGTH // SPAN
    factor = jnp.exp(jax.random.uniform(key_sequence[0], (HEAD_COUNT, spans), jnp.float32, math.log(0.4), math.log(2.5)))
    stable_level = jnp.repeat(factor, SPAN, axis=1) * (0.6 / SEQUENCE_LENGTH)
    spike_locations = jax.random.randint(key_sequence[1], (HEAD_COUNT, 3), 0, SEQUENCE_LENGTH)
    spike_depth = jax.random.uniform(key_sequence[2], (HEAD_COUNT, 3), jnp.float32, 0.22, 0.6)
    position_index = jnp.arange(SEQUENCE_LENGTH, dtype=jnp.int32)
    spike_hits = (position_index[None, None, :] == spike_locations[:, :, None]).astype(jnp.float32)
    spike_events = jnp.sum(spike_hits * spike_depth[:, :, None], axis=1)
    return (-(stable_level + spike_events)).astype(jnp.float32)


def steps_of(key, dims, pieces, least, high):
    loudness = 1.0
    for dim, blocks in pieces:
        heights = jax.random.uniform(jax.random.fold_in(jax.random.fold_in(key, 6), dim), (blocks,), jnp.float32, least / len(pieces), high / len(pieces))
        loudness = loudness * jnp.repeat(jnp.exp(heights), dims[dim] // blocks).reshape((-1,) + (1,) * (len(dims) - 1 - dim))
    return loudness


def shared_out(rng, own, number, rows, number_of, top, limit, skew):
    order = jax.random.permutation(rng, number_of)
    heavy_load, common = shares(number_of, rows * top, limit, skew, True), shares(number_of, rows * top, limit, skew, False)
    places = jnp.arange(number_of)

    def named(tallies, rotation):
        used = int((tallies > 0).sum())
        fixed = max(1, used // 4)
        moved = fixed + (places - fixed + rotation * (used - fixed)) % max(1, number_of - fixed)
        return jnp.zeros((number_of,), jnp.int32).at[order[jnp.where(places < fixed, places, moved)]].set(jnp.asarray(tallies, jnp.int32))

    tallies = jnp.where(number % 4 == 0, named(heavy_load, number // 4), named(common, number - number // 4 - 1))
    mixed = jax.random.permutation(jax.random.fold_in(own, 3), number_of)
    donor, taker = mixed[0:number_of // 2 * 2:2], mixed[1:number_of // 2 * 2:2]
    slack = jnp.minimum(tallies[donor] - 1, limit - tallies[taker]) // 2
    slack = jnp.where((donor == order[0]) | (taker == order[0]) | (tallies[taker] == 0), 0, jnp.maximum(slack, 0))
    moved = jax.random.randint(jax.random.fold_in(own, 4), (number_of // 2,), 0, 1 << 20) % (slack + 1)
    tallies = tallies.at[donor].add(-moved).at[taker].add(moved)
    labels = jnp.searchsorted(jnp.cumsum(tallies), jnp.arange(rows * top), side="right").astype(jnp.int32)
    grid = labels.reshape(top, rows).T
    grid = grid[jax.random.permutation(jax.random.fold_in(own, 1), rows)]
    rotation = jax.random.randint(jax.random.fold_in(own, 2), (rows, 1), 0, top)
    return jnp.take_along_axis(grid, (jnp.arange(top)[None, :] + rotation) % top, axis=1)


def shares(number_of, total, most, slope, full):
    weights = [(1 << 20) // math.isqrt(standing ** slope) + 1 for standing in range(1, number_of + 1)]
    largest = most if full else min(most, max(-(-total // number_of), total * weights[0] // sum(weights)))
    least = 1 if total - largest >= number_of - 1 else 0
    given, rest = [largest] + [least] * (number_of - 1), total - largest - least * (number_of - 1)
    while rest > 0:
        candidates = [i for i in range(1, number_of) if given[i] < largest] or [i for i in range(1, number_of) if given[i] < most]
        whole, remaining = sum([weights[i] for i in candidates]), rest
        for i in candidates:
            more = min(most - given[i], max(1, remaining * weights[i] // whole), rest)
            given[i] = given[i] + more
            rest = rest - more
    return np.array(given)


def normal_values(key, extent, scale, most, shards=(), held_as=jnp.bfloat16):
    factor_of = steps_of(key, extent, shards, -0.22, 0.18) if shards else 1.0
    drawn = jax.random.normal(key, extent, jnp.float32) * scale * factor_of
    return jnp.minimum(jnp.maximum(drawn, -most), most).astype(held_as)


def setup_inputs(seed: int = 0, part: int = 0) -> dict:
    streams_of = jax.random.split(jax.random.key(seed), 22)
    own_keys = jax.random.split(jax.random.fold_in(streams_of[21], part), 22)
    mix_rows = normal_values(own_keys[0], (SEQUENCE_LENGTH, D), 1.0, 6.0, ((0, 16),))
    expert_rows = normal_values(own_keys[1], (SEQUENCE_LENGTH, D), 1.0, 6.0, ((0, 16),))
    mix_gain = jnp.clip(1.0 + 0.18 * jax.random.normal(streams_of[2], (D,), jnp.float32), 0.1, 1.9)
    ffn_gain = jnp.clip(1.0 + 0.18 * jax.random.normal(streams_of[3], (D,), jnp.float32), 0.1, 1.9)
    w_query = normal_values(streams_of[4], (D, HEAD_COUNT * DK), D ** -0.5, 0.125, ((1, 4),))
    w_key = normal_values(streams_of[5], (D, HEAD_COUNT * DK), D ** -0.5, 0.125, ((1, 4),))
    w_value = normal_values(streams_of[6], (D, HEAD_COUNT * DV), D ** -0.5, 0.125, ((1, 4),))
    w_lowrank = normal_values(streams_of[7], (D, LOWRANK), D ** -0.5, 0.125)
    w_decay = normal_values(streams_of[8], (LOWRANK, HEAD_COUNT * DK), LOWRANK ** -0.5, 1.0)
    decay_bias = draw_decay_bias(jax.random.fold_in(streams_of[21], 71), part)
    decay_shift = draw_decay_shift(jax.random.fold_in(jax.random.fold_in(streams_of[21], part), 71), part)
    head_gain = jnp.clip(1.0 + 0.18 * jax.random.normal(streams_of[11], (DV,), jnp.float32), 0.1, 1.9)
    w_output = normal_values(streams_of[12], (HEAD_COUNT * DV, D), (HEAD_COUNT * DV) ** -0.5, 0.1875, ((0, 4),))
    route_ids_keys = jax.random.split(jax.random.fold_in(own_keys[13], 1), SEQUENCE_LENGTH // TOK_DEV)
    route_ids_turns = jax.random.permutation(jax.random.fold_in(own_keys[13], 3), SEQUENCE_LENGTH // TOK_DEV)
    route_ids = jax.vmap(lambda own, number: shared_out(jax.random.fold_in(own_keys[13], 2), own, number, TOK_DEV, EXPERTS, TOP_K, CAP, 2))(route_ids_keys, route_ids_turns).reshape((SEQUENCE_LENGTH, TOP_K))
    route_weights = jnp.clip(0.3 + 0.90000004 * jax.random.uniform(own_keys[14], (SEQUENCE_LENGTH, TOP_K), jnp.float32) ** steps_of(own_keys[14], (SEQUENCE_LENGTH, TOP_K), ((0, 16),), -0.2, 0.2), 0.3, 1.2)
    w_gate = normal_values(streams_of[15], (EXPERTS, D, FF), D ** -0.5, 0.125, ((0, 16),))
    w_lift = normal_values(streams_of[16], (EXPERTS, D, FF), D ** -0.5, 0.125, ((0, 16),))
    w_drop = normal_values(streams_of[17], (EXPERTS, FF, D), FF ** -0.5, 0.25, ((0, 16),))
    shared_gate = normal_values(streams_of[18], (D, FF), D ** -0.5, 0.125, ((1, 4),))
    shared_lift = normal_values(streams_of[19], (D, FF), D ** -0.5, 0.125, ((1, 4),))
    shared_drop = normal_values(streams_of[20], (FF, D), FF ** -0.5, 0.25, ((0, 4),))
    return {"mix_rows": mix_rows, "expert_rows": expert_rows, "mix_gain": mix_gain, "ffn_gain": ffn_gain, "w_query": w_query, "w_key": w_key, "w_value": w_value, "w_lowrank": w_lowrank, "w_decay": w_decay, "decay_bias": decay_bias, "decay_shift": decay_shift, "head_gain": head_gain, "w_output": w_output, "route_ids": route_ids, "route_weights": route_weights, "w_gate": w_gate, "w_lift": w_lift, "w_drop": w_drop, "shared_gate": shared_gate, "shared_lift": shared_lift, "shared_drop": shared_drop}


epsilon = 1e-05
gate_norm = 16.0
highest = lax.Precision.HIGHEST

def layer_norm(source, gain):
    values = source.astype(jnp.float32)
    center = values - lax.optimization_barrier(jnp.mean(values, axis=-1, keepdims=True))
    inverse = lax.rsqrt(lax.optimization_barrier(jnp.mean(center * center, axis=-1, keepdims=True)) + epsilon)
    return (center * inverse * gain).astype(jnp.bfloat16)

def stored(product):
    return lax.optimization_barrier(product.astype(jnp.bfloat16)).astype(jnp.float32)

def head_norm(attended, head_gain):
    inverse = lax.rsqrt(lax.optimization_barrier(jnp.mean(attended * attended, axis=-1, keepdims=True)) + epsilon)
    return (attended * inverse * head_gain).astype(jnp.bfloat16)

def gla_blocks(queries, key_rows, value_rows, log_decay, state_init):
    length, heads_here, key_width = queries.shape
    value_width = value_rows.shape[-1]
    blocks = length // BLOCK
    query_blocks = queries.reshape(blocks, BLOCK, heads_here, key_width)
    key_blocks = key_rows.reshape(blocks, BLOCK, heads_here, key_width)
    value_blocks = value_rows.reshape(blocks, BLOCK, heads_here, value_width)
    within = jnp.cumsum(log_decay.reshape(blocks, BLOCK, heads_here, key_width), axis=1)
    block_total = within[:, -1]
    scaled_query = query_blocks * jnp.exp(within)
    scaled_key = key_blocks * jnp.exp(-within)
    causal = jnp.tril(jnp.ones((BLOCK, BLOCK), dtype=jnp.bool_))
    scores = jnp.einsum('nihd,njhd->nhij', scaled_query, scaled_key, precision=highest)
    scores = jnp.where(causal, scores, 0.0)
    inside = jnp.einsum('nhij,njhv->nihv', scores, value_blocks, precision=highest)
    block_added = jnp.einsum('njhd,njhv->nhdv', key_blocks * jnp.exp(block_total[:, None] - within), value_blocks, precision=highest)

    def advance(state, inputs):
        decay_sum, addition = inputs
        return (jnp.exp(decay_sum)[:, :, None] * state + addition, state)
    final_state, entering = lax.scan(advance, state_init, (block_total, block_added))
    inside = inside + jnp.einsum('nihd,nhdv->nihv', scaled_query, entering, precision=highest)
    before = jnp.cumsum(block_total, axis=0) - block_total
    carried_query = query_blocks * jnp.exp(within + before[:, None])
    return (inside.reshape(length, heads_here, value_width), final_state, carried_query.reshape(length, heads_here, key_width), lax.optimization_barrier(jnp.sum(block_total, axis=0)))

def reference(mix_rows, expert_rows, mix_gain, ffn_gain, w_query, w_key, w_value, w_lowrank, w_decay, decay_bias, decay_shift, head_gain, w_output, route_ids, route_weights, w_gate, w_lift, w_drop, shared_gate, shared_lift, shared_drop):
    mix_normed = layer_norm(mix_rows, mix_gain)
    length = mix_normed.shape[0]
    queries = stored(jnp.dot(mix_normed, w_query, preferred_element_type=jnp.float32)).reshape(length, HEAD_COUNT, DK) * DK ** (-0.5)
    key_rows = stored(jnp.dot(mix_normed, w_key, preferred_element_type=jnp.float32)).reshape(length, HEAD_COUNT, DK)
    value_rows = stored(jnp.dot(mix_normed, w_value, preferred_element_type=jnp.float32)).reshape(length, HEAD_COUNT, DV)
    lowrank = jnp.dot(mix_normed, w_lowrank, preferred_element_type=jnp.float32).astype(jnp.bfloat16)
    logits = jnp.dot(lowrank, w_decay, preferred_element_type=jnp.float32) + decay_bias
    log_decay = jax.nn.log_sigmoid(logits).reshape(length, HEAD_COUNT, DK) / gate_norm + jnp.transpose(decay_shift)[:, :, None]
    gla_result = gla_blocks(queries, key_rows, value_rows, log_decay, jnp.zeros((HEAD_COUNT, DK, DV), jnp.float32))
    head_rows = head_norm(gla_result[0], head_gain).reshape(length, HEAD_COUNT * DV)
    group_width = HEAD_COUNT // N_TP * DV
    mixed = jnp.zeros((length, D), jnp.float32)
    for group_index in range(N_TP):
        first_row = group_index * group_width
        group_term = jnp.dot(head_rows[:, first_row:first_row + group_width], w_output[first_row:first_row + group_width], preferred_element_type=jnp.float32)
        mixed = mixed + group_term.astype(jnp.bfloat16).astype(jnp.float32)
    mixed = mixed.astype(jnp.bfloat16)
    expert_normed = layer_norm(expert_rows, ffn_gain)
    shared_hidden = (jax.nn.silu(jnp.dot(expert_normed, shared_gate, preferred_element_type=jnp.float32)) * jnp.dot(expert_normed, shared_lift, preferred_element_type=jnp.float32)).astype(jnp.bfloat16)
    unit_width = FF // N_TP
    shared_sum = jnp.zeros((length, D), jnp.float32)
    for group_index in range(N_TP):
        first_unit = group_index * unit_width
        unit_term = jnp.dot(shared_hidden[:, first_unit:first_unit + unit_width], shared_drop[first_unit:first_unit + unit_width], preferred_element_type=jnp.float32)
        shared_sum = shared_sum + unit_term.astype(jnp.bfloat16).astype(jnp.float32)
    flat_routes = route_ids.reshape(-1).astype(jnp.int32)
    expert_ids = jnp.arange(EXPERTS, dtype=jnp.int32)
    matches = (flat_routes[:, None] == expert_ids[None, :]).astype(jnp.int32)
    slot_rank = lax.optimization_barrier(jnp.sum((jnp.cumsum(matches, axis=0) - 1) * matches, axis=1)).astype(jnp.int32)
    slot_count = CAP * N_EP * N_TP
    token_index = jnp.arange(length * TOP_K, dtype=jnp.int32) // TOP_K
    slot_token = jnp.full((EXPERTS, slot_count), length, jnp.int32).at[flat_routes, slot_rank].set(token_index)
    slot_weight = jnp.zeros((EXPERTS, slot_count), jnp.float32).at[flat_routes, slot_rank].set(route_weights.reshape(-1).astype(jnp.float32))
    padded = jnp.concatenate([expert_normed, jnp.zeros((1, D), jnp.bfloat16)], axis=0)

    def one_expert(summed, inputs):
        token_slots, weight_slots, gate_matrix, lift_matrix, drop_matrix = inputs
        gathered = padded[token_slots]
        inner = (jax.nn.silu(jnp.dot(gathered, gate_matrix, preferred_element_type=jnp.float32)) * jnp.dot(gathered, lift_matrix, preferred_element_type=jnp.float32)).astype(jnp.bfloat16)
        result = stored(jnp.dot(inner, drop_matrix, preferred_element_type=jnp.float32))
        return (summed.at[token_slots].add(weight_slots[:, None] * result), None)
    routed, unused = lax.scan(one_expert, jnp.zeros((length + 1, D), jnp.float32), (slot_token, slot_weight, w_gate, w_lift, w_drop))
    expert_out = (shared_sum + routed[:length]).astype(jnp.bfloat16)
    return (mixed, expert_out)
```

```python
import functools

import jax
import jax.numpy as jnp
from jax import lax
from jax.experimental import pallas as pl
from jax.experimental.pallas import tpu as pltpu
from jax.sharding import PartitionSpec as P

DK = 64
DV = 128
BLOCK = 64


epsilon = 1e-05
gate_norm = 16.0
highest = lax.Precision.HIGHEST


def entering_2(value, axis, combine, identity):
    length, mine = (lax.axis_size(axis), lax.axis_index(axis))
    everything = jax.tree.map(
        lambda part, kind: lax.all_gather(part.astype(kind), axis),
        value,
        (jnp.bfloat16, jnp.bfloat16),
    )
    start = jax.tree.map(
        lambda part, zero: jnp.broadcast_to(jnp.asarray(zero, part.dtype), part.shape),
        value,
        identity,
    )

    def lap(k, before):
        reached = k < mine
        new = combine(
            before, jax.tree.map(lambda part, own: part[k].astype(own.dtype), everything, value)
        )
        return jax.tree.map(lambda a, b: jnp.where(reached, a, b), new, before)

    return lax.fori_loop(0, length, lap, start)


def layer_norm(source, gain):
    values = source.astype(jnp.float32)
    center = values - jnp.mean(values, axis=-1, keepdims=True)
    inverse = lax.rsqrt(jnp.mean(center * center, axis=-1, keepdims=True) + epsilon)
    return (center * inverse * gain).astype(jnp.bfloat16)


def exchange(block, distance):
    pairs = [(source, source ^ distance) for source in range(lax.axis_size("tp"))]
    return lax.ppermute(block, "tp", pairs)


def shifted(block, steps):
    length = lax.axis_size("ep")
    return lax.ppermute(block, "ep", [(k, (k + steps) % length) for k in range(length)])


def distances():
    count = lax.axis_size("tp")
    found = []
    while count > 1:
        count //= 2
        found.append(count)
    return found


def spread(block):
    blocks = {0: block}
    for distance in distances():
        blocks.update({rel ^ distance: exchange(part, distance) for rel, part in list(blocks.items())})
    return blocks


def collect_split(near, far):
    count = lax.axis_size("tp")
    got = exchange(far, 1).astype(jnp.float32)
    parts = jnp.split(near.astype(jnp.float32) + got, count // 2, axis=0)
    blocks = dict(zip(range(0, count, 2), parts))
    for distance in reversed(distances()[:-1]):
        away = [rel for rel in blocks if rel & distance]
        sent = [exchange(blocks[rel].astype(jnp.bfloat16), distance) for rel in away]
        blocks = {
            rel ^ distance: blocks[rel ^ distance] + part.astype(jnp.float32)
            for rel, part in zip(away, sent)
        }
    return blocks[0]


def matmul(a, b, precision=None, dims=((1,), (0,))):
    return lax.dot_general(
        a, b, (dims, ((), ())), precision=precision, preferred_element_type=jnp.float32
    )


def mixer_kernel(count, heads, *refs):
    mine_ref, rows_refs = refs[0], refs[1 : 1 + count]
    w_query, w_key, w_value, w_lowrank, decay_cols, bias, shift = refs[1 + count : 8 + count]
    inside_ref, carried_ref, packed_ref = refs[8 + count : 11 + count]
    query_s, key_s, value_s, decay_s = refs[11 + count :]
    own = rows_refs[0].shape[0]
    for rel, rows_ref in enumerate(rows_refs):
        place = pl.ds(pl.multiple_of((mine_ref[0] ^ rel) * own, own), own)
        rows = rows_ref[...]
        rounded = matmul(rows, w_query[...]).astype(jnp.bfloat16).astype(jnp.float32)
        query_s[place, :] = rounded * DK ** (-0.5)
        key_s[place, :] = matmul(rows, w_key[...]).astype(jnp.bfloat16).astype(jnp.float32)
        value_s[place, :] = matmul(rows, w_value[...]).astype(jnp.bfloat16).astype(jnp.float32)
        lowrank = matmul(rows, w_lowrank[...]).astype(jnp.bfloat16)
        logits = matmul(lowrank, decay_cols[...]) + bias[...]
        log_sig = jnp.minimum(logits, 0.0) - jnp.log1p(jnp.exp(-jnp.abs(logits)))
        decay_s[place, :] = log_sig / gate_norm + shift[place, :]
    at_row = lax.broadcasted_iota(jnp.int32, (BLOCK, BLOCK), 0)
    at_col = lax.broadcasted_iota(jnp.int32, (BLOCK, BLOCK), 1)
    causal = at_row >= at_col
    lower = causal.astype(jnp.float32)
    ones = jnp.ones((BLOCK, DV), jnp.float32)
    states = [jnp.zeros((DK, DV), jnp.float32) for _ in range(heads)]
    totals = [jnp.zeros((DK, DV), jnp.float32) for _ in range(heads)]
    before = jnp.zeros((1, heads * DK), jnp.float32)
    for block in range(query_s.shape[0] // BLOCK):
        place = slice(block * BLOCK, (block + 1) * BLOCK)
        query, key, decay = query_s[place, :], key_s[place, :], decay_s[place, :]
        within = matmul(lower, decay, highest)
        block_total = within[BLOCK - 1 :, :]
        scaled_query = query * jnp.exp(within)
        scaled_key = key * jnp.exp(-within)
        ending_key = key * jnp.exp(block_total - within)
        carried_ref[place, :] = query * jnp.exp(within + before)
        before = before + block_total
        for head in range(heads):
            cols = slice(head * DK, (head + 1) * DK)
            value = value_s[place, head * DV : (head + 1) * DV]
            scores = matmul(scaled_query[:, cols], scaled_key[:, cols], highest, ((1,), (1,)))
            inside = matmul(jnp.where(causal, scores, 0.0), value, highest)
            inside = inside + matmul(scaled_query[:, cols], states[head], highest)
            inside_ref[place, head * DV : (head + 1) * DV] = inside
            added = matmul(ending_key[:, cols], value, highest, ((0,), (0,)))
            total = matmul(decay[:, cols], ones, highest, ((0,), (0,)))
            states[head] = jnp.exp(total) * states[head] + added
            totals[head] = totals[head] + total
    for head in range(heads):
        packed_ref[head * DK : (head + 1) * DK, :DV] = states[head]
        packed_ref[head * DK : (head + 1) * DK, DV:] = totals[head]


def mixer(mine, blocks, w_query, w_key, w_value, w_lowrank, decay_cols, bias, shift):
    count, own = len(blocks), blocks[0].shape[0]
    span, key_cols, value_cols = count * own, w_query.shape[1], w_value.shape[1]
    heads = key_cols // DK
    f32 = jnp.float32
    whole = pl.BlockSpec(memory_space=pltpu.VMEM)
    return pl.pallas_call(
        functools.partial(mixer_kernel, count, heads),
        out_shape=(
            jax.ShapeDtypeStruct((span, value_cols), f32),
            jax.ShapeDtypeStruct((span, key_cols), f32),
            jax.ShapeDtypeStruct((key_cols, 2 * DV), f32),
        ),
        in_specs=[pl.BlockSpec(memory_space=pltpu.SMEM)] + [whole] * (count + 7),
        out_specs=(whole, whole, whole),
        scratch_shapes=[
            pltpu.VMEM((span, key_cols), f32),
            pltpu.VMEM((span, key_cols), f32),
            pltpu.VMEM((span, value_cols), f32),
            pltpu.VMEM((span, key_cols), f32),
        ],
        cost_estimate=pl.CostEstimate(
            flops=40_000_000_000, bytes_accessed=8_000_000, transcendentals=0
        ),
        name="mixer",
    )(mine, *blocks, w_query, w_key, w_value, w_lowrank, decay_cols, bias, shift)


def output_kernel(count, heads, mine_ref, inside, carried, entering, gain, w_output, near, far):
    own = inside.shape[0] // count
    for rel in range(count):
        place = pl.ds(pl.multiple_of((mine_ref[0] ^ rel) * own, own), own)
        pieces = []
        for head in range(heads):
            cols = slice(head * DK, (head + 1) * DK)
            attended = inside[place, head * DV : (head + 1) * DV] + matmul(
                carried[place, cols], entering[cols, :], highest
            )
            mean = jnp.mean(attended * attended, axis=-1, keepdims=True)
            pieces.append((attended * lax.rsqrt(mean + epsilon) * gain[...]).astype(jnp.bfloat16))
        terms = matmul(jnp.concatenate(pieces, axis=1), w_output[...]).astype(jnp.bfloat16)
        target = far if rel % 2 else near
        target[rel // 2 * own : (rel // 2 + 1) * own, :] = terms


def output_terms(mine, count, inside, carried, entering, gain, w_output):
    half = jax.ShapeDtypeStruct((inside.shape[0] // 2, w_output.shape[1]), jnp.bfloat16)
    whole = pl.BlockSpec(memory_space=pltpu.VMEM)
    return pl.pallas_call(
        functools.partial(output_kernel, count, entering.shape[0] // DK),
        out_shape=(half, half),
        in_specs=[pl.BlockSpec(memory_space=pltpu.SMEM)] + [whole] * 5,
        out_specs=(whole, whole),
        cost_estimate=pl.CostEstimate(
            flops=5_000_000_000, bytes_accessed=4_000_000, transcendentals=0
        ),
        name="output_terms",
    )(mine, inside, carried, entering, gain, w_output)


def expert_kernel(count, experts, width, has_shared, *refs):
    first_ref, rows_refs = refs[0], refs[1 : 1 + count]
    w_gate, w_lift, w_drop = refs[1 + count : 4 + count]
    near, far, rows_s, total_s = refs[-4:]
    own = rows_refs[0].shape[0]
    local, tile = pl.program_id(0), pl.program_id(1)

    @pl.when((local == 0) & (tile == 0))
    def _():
        for rel, rows_ref in enumerate(rows_refs):
            rows_s[rel * own : (rel + 1) * own, :] = rows_ref[...]
        if has_shared:
            gate, lift, drop = refs[4 + count : 7 + count]
            rows = rows_s[:, :width]
            inner = jax.nn.silu(matmul(rows, gate[...])) * matmul(rows, lift[...])
            total_s[...] = matmul(inner.astype(jnp.bfloat16), drop[...])
        else:
            total_s[...] = jnp.zeros_like(total_s)

    rows = rows_s[:, :width]
    tail = rows_s[:, width:].astype(jnp.float32)
    lane = lax.broadcasted_iota(jnp.int32, tail.shape, 1)
    wanted = (lane < 3 * experts) & (lax.rem(lane, experts) == first_ref[0] + local)
    column = jnp.sum(jnp.where(wanted, tail, 0.0), axis=1, keepdims=True)
    gate_part = matmul(rows, w_gate[0])
    inner = (gate_part / (1.0 + jnp.exp(-gate_part)) * matmul(rows, w_lift[0])).astype(jnp.bfloat16)
    total_s[...] += column * matmul(inner, w_drop[0])

    @pl.when((local == pl.num_programs(0) - 1) & (tile == pl.num_programs(1) - 1))
    def _():
        for rel in range(count):
            target = far if rel % 2 else near
            part = total_s[rel * own : (rel + 1) * own, :].astype(jnp.bfloat16)
            target[rel // 2 * own : (rel // 2 + 1) * own, :] = part


def expert_terms(first, blocks, experts, weights, shared):
    count, (own, padded_width) = len(blocks), blocks[0].shape
    w_gate, w_lift, w_drop = weights
    local_experts, width, hidden = w_gate.shape
    tiles = 2 if hidden % 256 == 0 else 1
    piece = hidden // tiles
    half = jax.ShapeDtypeStruct((count * own // 2, width), jnp.bfloat16)

    def same(array):
        return pl.BlockSpec(array.shape, lambda l, j: (0, 0))

    return pl.pallas_call(
        functools.partial(expert_kernel, count, experts, width, bool(shared)),
        out_shape=(half, half),
        grid=(local_experts, tiles),
        in_specs=[pl.BlockSpec(memory_space=pltpu.SMEM)]
        + [same(block) for block in blocks]
        + [
            pl.BlockSpec((1, width, piece), lambda l, j: (l, 0, j)),
            pl.BlockSpec((1, width, piece), lambda l, j: (l, 0, j)),
            pl.BlockSpec((1, piece, width), lambda l, j: (l, j, 0)),
        ]
        + [same(array) for array in shared],
        out_specs=(same(half), same(half)),
        scratch_shapes=[
            pltpu.VMEM((count * own, padded_width), jnp.bfloat16),
            pltpu.VMEM((count * own, width), jnp.float32),
        ],
        cost_estimate=pl.CostEstimate(
            flops=10_000_000_000, bytes_accessed=10_000_000, transcendentals=0
        ),
        name="expert_terms",
    )(first, *blocks, *weights, *shared)


def entering_direct(packed):
    length, mine = lax.axis_size("ep"), lax.axis_index("ep")
    width = packed.shape[-1] // 2
    state = jnp.zeros((packed.shape[0], width), jnp.float32)
    for steps in range(length - 1, 0, -1):
        got = lax.ppermute(packed, "ep", [(k, k + steps) for k in range(length - steps)])
        state = jnp.where(
            mine >= steps, jnp.exp(got[:, width:]) * state + got[:, :width], state
        )
    return state


def dense_weights(route_ids, route_weights, experts):
    named = route_ids[:, :, None] == jnp.arange(experts, dtype=route_ids.dtype)
    return jnp.sum(jnp.where(named, route_weights[:, :, None], 0.0), axis=1)


def experts_dense(expert_normed, route_ids, route_weights, weights, shared):
    spans, local_experts = lax.axis_size("ep"), weights[0].shape[0]
    experts = spans * lax.axis_size("tp") * local_experts
    first = (lax.axis_index("ep") * lax.axis_size("tp") + lax.axis_index("tp")) * local_experts
    chosen = dense_weights(route_ids, route_weights, experts)
    high = lax.reduce_precision(chosen, 8, 7)
    middle = lax.reduce_precision(chosen - high, 8, 7)
    low = chosen - high - middle
    extra = jnp.concatenate([high, middle, low], axis=1).astype(jnp.bfloat16)
    extra = jnp.pad(extra, ((0, 0), (0, -extra.shape[1] % 128)))
    moving = jnp.concatenate([expert_normed, extra], axis=1)
    total = None
    for step in range(spans):
        if step:
            moving = shifted(moving, 1)
        blocks = spread(moving)
        near, far = expert_terms(
            first[None],
            [blocks[rel] for rel in sorted(blocks)],
            experts,
            weights,
            () if step else shared,
        )
        mine = collect_split(near, far)
        if step:
            mine = shifted(mine.astype(jnp.bfloat16), -step).astype(jnp.float32)
        total = mine if total is None else total + mine
    return total.astype(jnp.bfloat16)


def body(
    mix_rows,
    expert_rows,
    mix_gain,
    ffn_gain,
    w_query,
    w_key,
    w_value,
    w_lowrank,
    w_decay,
    decay_bias,
    decay_shift,
    head_gain,
    w_output,
    route_ids,
    route_weights,
    w_gate,
    w_lift,
    w_drop,
    shared_gate,
    shared_lift,
    shared_drop,
):
    mix_normed = layer_norm(mix_rows, mix_gain)
    local_heads = w_query.shape[1] // DK
    key_cols = local_heads * DK
    column = lax.axis_index("tp") * key_cols
    decay_cols = lax.dynamic_slice_in_dim(w_decay, column, key_cols, 1)
    bias_cols = lax.dynamic_slice_in_dim(decay_bias, column, key_cols, 0)
    found = spread(mix_normed)
    mine = lax.axis_index("tp")[None]
    inside, carried_query, packed = mixer(
        mine,
        [found[rel] for rel in sorted(found)],
        w_query,
        w_key,
        w_value,
        w_lowrank,
        decay_cols,
        bias_cols[None],
        jnp.repeat(jnp.transpose(decay_shift), DK, axis=1),
    )
    own_tokens, top_count = route_ids.shape
    devices = lax.axis_size("ep") * lax.axis_size("tp")
    dense = devices <= 4 * top_count

    def chain(earlier, later):
        return (earlier[0] + later[0], jnp.exp(later[0])[:, :, None] * earlier[1] + later[1])

    if dense:
        entering = entering_direct(packed)
    else:
        states = packed.reshape(local_heads, DK, 2 * DV)
        decay_total, final_state = states[:, :, DV], states[:, :, :DV]
        entering = entering_2(
            (decay_total, final_state),
            "ep",
            chain,
            (jnp.zeros_like(decay_total), jnp.zeros_like(final_state)),
        )[1].reshape(local_heads * DK, DV)
    near, far = output_terms(
        mine, len(found), inside, carried_query, entering, head_gain[None], w_output
    )
    mixed = collect_split(near, far).astype(jnp.bfloat16)
    expert_normed = layer_norm(expert_rows, ffn_gain)
    if dense:
        combined = experts_dense(
            expert_normed,
            route_ids,
            route_weights,
            (w_gate, w_lift, w_drop),
            (shared_gate, shared_lift, shared_drop),
        )
        return (mixed, combined)
    shard_rows = lax.all_gather(expert_normed, "tp", axis=0, tiled=True)
    hidden = (
        jax.nn.silu(jnp.dot(shard_rows, shared_gate, preferred_element_type=jnp.float32))
        * jnp.dot(shard_rows, shared_lift, preferred_element_type=jnp.float32)
    ).astype(jnp.bfloat16)
    shared_sum = lax.psum_scatter(
        jnp.dot(hidden, shared_drop, preferred_element_type=jnp.float32).astype(jnp.bfloat16),
        "tp",
        scatter_dimension=0,
        tiled=True,
    ).astype(jnp.float32)
    local_experts = w_gate.shape[0]
    experts = lax.axis_size("ep") * lax.axis_size("tp") * local_experts
    capacity = 2 * own_tokens * top_count // experts
    flat_routes = route_ids.reshape(-1)
    matches = (flat_routes[:, None] == jnp.arange(experts, dtype=jnp.int32)[None, :]).astype(
        jnp.int32
    )
    slot_rank = jnp.sum((jnp.cumsum(matches, axis=0) - 1) * matches, axis=1)
    slot_index = flat_routes * capacity + slot_rank
    token_index = jnp.arange(own_tokens * top_count, dtype=jnp.int32) // top_count
    slot_token = (
        jnp.full((experts * capacity,), own_tokens, jnp.int32).at[slot_index].set(token_index)
    )
    padded = jnp.concatenate(
        [expert_normed, jnp.zeros((1, expert_normed.shape[1]), jnp.bfloat16)], axis=0
    )
    outgoing = padded[slot_token].reshape(experts, capacity, -1)
    arrived = lax.all_to_all(outgoing, ("ep", "tp"), split_axis=0, concat_axis=0, tiled=True)
    arrived_shape = arrived.shape
    grouped = arrived.reshape(-1, local_experts, arrived_shape[-2], arrived_shape[-1])
    gate_part = jnp.einsum("sepd,edf->sepf", grouped, w_gate, preferred_element_type=jnp.float32)
    lift_part = jnp.einsum("sepd,edf->sepf", grouped, w_lift, preferred_element_type=jnp.float32)
    inner = (jax.nn.silu(gate_part) * lift_part).astype(jnp.bfloat16)
    result = jnp.einsum("sepf,efd->sepd", inner, w_drop, preferred_element_type=jnp.float32)
    returned = lax.all_to_all(
        result.astype(jnp.bfloat16).reshape(arrived_shape),
        ("ep", "tp"),
        split_axis=0,
        concat_axis=0,
        tiled=True,
    )
    results = returned.reshape(experts * capacity, -1)[slot_index].reshape(
        own_tokens, top_count, -1
    )
    combined = shared_sum + jnp.sum(route_weights[:, :, None] * results.astype(jnp.float32), axis=1)
    return (mixed, combined.astype(jnp.bfloat16))


def solution(mesh):
    return jax.shard_map(
        body,
        mesh=mesh,
        in_specs=(
            P(("grp", "ep", "tp"), None),
            P(("grp", "ep", "tp"), None),
            P(),
            P(),
            P(None, "tp"),
            P(None, "tp"),
            P(None, "tp"),
            P(),
            P(),
            P(),
            P("tp", ("grp", "ep")),
            P(),
            P("tp", None),
            P(("grp", "ep", "tp"), None),
            P(("grp", "ep", "tp"), None),
            P(("ep", "tp"), None, None),
            P(("ep", "tp"), None, None),
            P(("ep", "tp"), None, None),
            P(None, "tp"),
            P(None, "tp"),
            P("tp", None),
        ),
        out_specs=(P(("grp", "ep", "tp"), None), P(("grp", "ep", "tp"), None)),
        check_vma=False,
    )
```
